128 devices in a mesh: ep: 64 (over z, y, x), tp: 2 (over core).
Axes of the slice: x: 4, y: 4, z: 4, core: 2. Of those that a mesh axis runs over, the one named last changes fastest.
Arguments:
- inputs: bfloat16 [4096, 2048], P('ep'), may hold values from -6 to 6
- cache_keys: bfloat16 [4096, 2, 64, 1024], P('ep', 'tp'), may hold values from -6 to 6
- cache_values: bfloat16 [4096, 2, 64, 1024], P('ep', 'tp'), may hold values from -12 to 12
- lengths: int32 [4096], P('ep'), may hold values from 1 to 1024, as said below
- query_weight: bfloat16 [2048, 1024], P(None, 'tp'), may hold values from -0.125 to 0.125
- key_weight: bfloat16 [2048, 128], P(None, 'tp'), may hold values from -0.125 to 0.125
- value_weight: bfloat16 [2048, 128], P(None, 'tp'), may hold values from -0.125 to 0.125
- head_bias: float32 [16], P('tp'), may hold values from -7 to -3
- out_weight: bfloat16 [1024, 2048], P('tp'), may hold values from -0.75 to 0.75
- attend_gain: float32 [2048], replicated, may hold values from 0.1 to 1.9
- router_weight: bfloat16 [2048, 64], replicated, may hold values from -0.125 to 0.125
- routes: int32 [4096, 4], P('ep'), may hold values from 0 to 63, all different within a row; in each aligned block of 64 rows (0 to 63, 64 to 127, ...) at most 8 rows name the same one
- expert_gate: bfloat16 [64, 2048, 512], P('ep', None, 'tp'), may hold values from -0.125 to 0.125
- expert_up: bfloat16 [64, 2048, 512], P('ep', None, 'tp'), may hold values from -0.125 to 0.125
- expert_down: bfloat16 [64, 512, 2048], P('ep', 'tp'), may hold values from -0.25 to 0.25
- shared_gate: bfloat16 [2048, 512], P(None, 'tp'), may hold values from -0.125 to 0.125
- shared_up: bfloat16 [2048, 512], P(None, 'tp'), may hold values from -0.125 to 0.125
- shared_down: bfloat16 [512, 2048], P('tp'), may hold values from -0.25 to 0.25
- final_gain: float32 [2048], P('tp'), may hold values from 0.1 to 1.9
Outputs:
- output: bfloat16 [4096, 2048], P('ep', 'tp')
- new_keys: bfloat16 [4096, 128], P('ep', 'tp')
- new_values: bfloat16 [4096, 128], P('ep', 'tp')
The draws below stay inside these ranges and needn't reach their ends.
Inputs may be any that keep to these rules, and one draw needn't show every extreme that they name: `lengths`: some sequence has 1024 filled positions and some other has 1. `routes`: each row names 4 different experts. Among the 64 rows of one index of ep no expert is named more than 8 times; some expert is named exactly 8 times by the rows of some index.
All inputs are finite; a program needn't handle non-finite values.
Results may differ from the reference program's by a relative error of at most 0.015.
Values may be sent and summed in bfloat16 or wider, within the bound.
No kernel may reach another device: no remote copies, remote signals or barrier semaphores. Data moves between devices by JAX's collectives and lax.ppermute only.
A program may use at most 128 MiB of HBM per device.

```python
import math
import jax
import jax.numpy as jnp
import numpy as np
from jax import lax

D = 2048
HEAD = 64
Q_HEADS = 16
KV_HEADS = 2
FF_EXP = 512
FF_SH = 512
TOPK = 4
SEQ_DEV = 64
CACHE = 1024
SEQS = 4096
EXPERTS = 64
CAP = 8
N_EP = 64
N_TP = 2


def draw_lengths(key, part):
    first_key = jax.random.fold_in(key, 11)
    second_key = jax.random.fold_in(key, 12)
    third_key = jax.random.fold_in(key, 13)
    blocks = SEQS // SEQ_DEV
    limits = jax.random.randint(first_key, (blocks, 1), CACHE // 8, CACHE + 1)
    spread = jax.random.randint(second_key, (blocks, SEQ_DEV), 0, CACHE)
    filled = (1 + spread % limits).reshape(SEQS)
    order = jax.random.permutation(third_key, SEQS)
    filled = filled.at[order[0]].set(CACHE).at[order[1]].set(1)
    return filled.astype(jnp.int32)


def shard_levels(own_key, shape, cuts, least, top_value):
    loudness = 1.0
    for dim, parts in cuts:
        heights = jax.random.uniform(jax.random.fold_in(jax.random.fold_in(own_key, 6), dim), (parts,), jnp.float32, least / len(cuts), top_value / len(cuts))
        loudness = loudness * jnp.repeat(jnp.exp(heights), shape[dim] // parts).reshape((-1,) + (1,) * (len(shape) - 1 - dim))
    return loudness


def routed_block(stream_key, own, number, rows, amount, top, bound, lean):
    sequence = jax.random.permutation(stream_key, amount)
    heavy_load, common = shares(amount, rows * top, bound, lean, True), shares(amount, rows * top, bound, lean, False)
    places = jnp.arange(amount)

    def named(sizes, offset_by):
        used = int((sizes > 0).sum())
        fixed = max(1, used // 4)
        shifted = fixed + (places - fixed + offset_by * (used - fixed)) % max(1, amount - fixed)
        return jnp.zeros((amount,), jnp.int32).at[sequence[jnp.where(places < fixed, places, shifted)]].set(jnp.asarray(sizes, jnp.int32))

    sizes = jnp.where(number % 4 == 0, named(heavy_load, number // 4), named(common, number - number // 4 - 1))
    mixed = jax.random.permutation(jax.random.fold_in(own, 3), amount)
    giver, taker = mixed[0:amount // 2 * 2:2], mixed[1:amount // 2 * 2:2]
    slack = jnp.minimum(sizes[giver] - 1, bound - sizes[taker]) // 2
    slack = jnp.where((giver == sequence[0]) | (taker == sequence[0]) | (sizes[taker] == 0), 0, jnp.maximum(slack, 0))
    shifted = jax.random.randint(jax.random.fold_in(own, 4), (amount // 2,), 0, 1 << 20) % (slack + 1)
    sizes = sizes.at[giver].add(-shifted).at[taker].add(shifted)
    items = jnp.searchsorted(jnp.cumsum(sizes), jnp.arange(rows * top), side="right").astype(jnp.int32)
    table = items.reshape(top, rows).T
    table = table[jax.random.permutation(jax.random.fold_in(own, 1), rows)]
    offset_by = jax.random.randint(jax.random.fold_in(own, 2), (rows, 1), 0, top)
    return jnp.take_along_axis(table, (jnp.arange(top)[None, :] + offset_by) % top, axis=1)


def shares(amount, total, most, lean, full):
    weights = [(1 << 20) // math.isqrt(rank ** lean) + 1 for rank in range(1, amount + 1)]
    largest = most if full else min(most, max(-(-total // amount), total * weights[0] // sum(weights)))
    least = 1 if total - largest >= amount - 1 else 0
    counts, spare = [largest] + [least] * (amount - 1), total - largest - least * (amount - 1)
    while spare > 0:
        movable = [i for i in range(1, amount) if counts[i] < largest] or [i for i in range(1, amount) if counts[i] < most]
        mass, budget = sum([weights[i] for i in movable]), spare
        for i in movable:
            more = min(most - counts[i], max(1, budget * weights[i] // mass), spare)
            counts[i] = counts[i] + more
            spare = spare - more
    return np.array(counts)


def bell_draw(own_key, shape, scale, limit, split=(), kind=jnp.bfloat16):
    result = jax.random.normal(own_key, shape, jnp.float32) * scale
    if len(split) > 0:
        result = shard_levels(own_key, shape, split, -0.22, 0.18) * result
    return jnp.clip(result, min=-limit, max=limit).astype(kind)


def setup_inputs(seed: int = 0) -> dict:
    seeds = jax.random.split(jax.random.key(seed), 20)
    inputs = bell_draw(seeds[0], (SEQS, D), 1.0, 6.0, ((0, 64),))
    cache_keys = bell_draw(seeds[1], (SEQS, KV_HEADS, HEAD, CACHE), 1.0, 6.0, ((0, 64), (1, 2)))
    cache_values = bell_draw(seeds[2], (SEQS, KV_HEADS, HEAD, CACHE), 2.0, 12.0, ((0, 64), (1, 2)))
    lengths = draw_lengths(jax.random.fold_in(seeds[19], 71), 0)
    query_weight = bell_draw(seeds[4], (D, Q_HEADS * HEAD), D ** -0.5, 0.125, ((1, 2),))
    key_weight = bell_draw(seeds[5], (D, KV_HEADS * HEAD), D ** -0.5, 0.125, ((1, 2),))
    value_weight = bell_draw(seeds[6], (D, KV_HEADS * HEAD), D ** -0.5, 0.125, ((1, 2),))
    head_bias = jnp.clip(-7.0 + 4.0 * jax.random.uniform(seeds[7], (Q_HEADS,), jnp.float32) ** shard_levels(seeds[7], (Q_HEADS,), ((0, 2),), -0.2, 0.2), -7.0, -3.0)
    out_weight = bell_draw(seeds[8], (Q_HEADS * HEAD, D), HEAD ** -0.5, 0.75, ((0, 2),))
    attend_gain = jnp.clip(1.0 + 0.18 * jax.random.normal(seeds[9], (D,), jnp.float32), 0.1, 1.9)
    router_weight = bell_draw(seeds[10], (D, EXPERTS), D ** -0.5, 0.125)
    routes_keys = jax.random.split(jax.random.fold_in(seeds[11], 1), SEQS // SEQ_DEV)
    routes_turns = jax.random.permutation(jax.random.fold_in(seeds[11], 3), SEQS // SEQ_DEV)
    routes = jax.vmap(lambda own, number: routed_block(jax.random.fold_in(seeds[11], 2), own, number, SEQ_DEV, EXPERTS, TOPK, CAP, 2))(routes_keys, routes_turns).reshape((SEQS, TOPK))
    expert_gate = bell_draw(seeds[12], (EXPERTS, D, FF_EXP), D ** -0.5, 0.125, ((0, 64), (2, 2)))
    expert_up = bell_draw(seeds[13], (EXPERTS, D, FF_EXP), D ** -0.5, 0.125, ((0, 64), (2, 2)))
    expert_down = bell_draw(seeds[14], (EXPERTS, FF_EXP, D), FF_EXP ** -0.5, 0.25, ((0, 64), (1, 2)))
    shared_gate = bell_draw(seeds[15], (D, FF_SH), D ** -0.5, 0.125, ((1, 2),))
    shared_up = bell_draw(seeds[16], (D, FF_SH), D ** -0.5, 0.125, ((1, 2),))
    shared_down = bell_draw(seeds[17], (FF_SH, D), FF_SH ** -0.5, 0.25, ((0, 2),))
    final_gain = jnp.clip(1.0 + 0.18 * jax.random.normal(seeds[18], (D,), jnp.float32), 0.1, 1.9)
    return {"inputs": inputs, "cache_keys": cache_keys, "cache_values": cache_values, "lengths": lengths, "query_weight": query_weight, "key_weight": key_weight, "value_weight": value_weight, "head_bias": head_bias, "out_weight": out_weight, "attend_gain": attend_gain, "router_weight": router_weight, "routes": routes, "expert_gate": expert_gate, "expert_up": expert_up, "expert_down": expert_down, "shared_gate": shared_gate, "shared_up": shared_up, "shared_down": shared_down, "final_gain": final_gain}


RESIDUAL_SCALE = 2.0 ** 0.25
ROUTE_SCALE = 2.5
NORM_EPS = 1e-05

def layer_norm(values, gain_vec):
    row_mean = lax.optimization_barrier(jnp.mean(values, axis=-1, keepdims=True))
    centered = values - row_mean
    row_var = lax.optimization_barrier(jnp.mean(centered * centered, axis=-1, keepdims=True))
    return centered * lax.rsqrt(row_var + NORM_EPS) * gain_vec

def split_sum(inner_rows, weight_rows, pieces):
    total_rows, inner_width = inner_rows.shape
    left_parts = inner_rows.reshape(total_rows, pieces, inner_width // pieces).astype(jnp.float32)
    right_parts = weight_rows.reshape(pieces, inner_width // pieces, -1).astype(jnp.float32)
    partial_value = jnp.einsum('rpf,pfd->prd', left_parts, right_parts)
    rounded = lax.optimization_barrier(partial_value.astype(jnp.bfloat16))
    return lax.optimization_barrier(jnp.sum(rounded.astype(jnp.float32), axis=0))

def reference(inputs, cache_keys, cache_values, lengths, query_weight, key_weight, value_weight, head_bias, out_weight, attend_gain, router_weight, routes, expert_gate, expert_up, expert_down, shared_gate, shared_up, shared_down, final_gain):
    groups = Q_HEADS // KV_HEADS
    query = jnp.dot(inputs, query_weight, preferred_element_type=jnp.float32).astype(jnp.bfloat16)
    new_keys = jnp.dot(inputs, key_weight, preferred_element_type=jnp.float32).astype(jnp.bfloat16)
    new_values = jnp.dot(inputs, value_weight, preferred_element_type=jnp.float32).astype(jnp.bfloat16)
    query_heads = query.reshape(SEQS, KV_HEADS, groups, HEAD).astype(jnp.float32)
    scores = jnp.einsum('skgd,skdc->skgc', query_heads, cache_keys.astype(jnp.float32)) * HEAD ** (-0.5)
    scores = scores + head_bias.reshape(KV_HEADS, groups)[None, :, :, None]
    positions = jnp.arange(CACHE, dtype=jnp.int32)
    usable = positions[None, None, None, :] < lengths[:, None, None, None]
    log_keep = jnp.where(usable, jax.nn.log_sigmoid(-scores), 0.0)
    later_sum = lax.cumsum(log_keep, axis=3, reverse=True) - log_keep
    stick_weight = jnp.where(usable, jnp.exp(jax.nn.log_sigmoid(scores) + later_sum), 0.0).astype(jnp.bfloat16)
    attended = jnp.einsum('skgc,skdc->skgd', stick_weight.astype(jnp.float32), cache_values.astype(jnp.float32))
    attended = attended.astype(jnp.bfloat16).reshape(SEQS, Q_HEADS * HEAD)
    attention = split_sum(attended, out_weight, N_TP)
    hidden = layer_norm(RESIDUAL_SCALE * inputs.astype(jnp.float32) + attention, attend_gain).astype(jnp.bfloat16)
    router_probs = jax.nn.sigmoid(jnp.dot(hidden, router_weight, preferred_element_type=jnp.float32))
    chosen = jnp.take_along_axis(router_probs, routes, axis=1)
    route_weights = ROUTE_SCALE * chosen / lax.optimization_barrier(jnp.sum(chosen, axis=1, keepdims=True))
    block_routes = routes.reshape(N_EP, SEQ_DEV * TOPK)
    onehot_rows = (block_routes[:, :, None] == jnp.arange(EXPERTS, dtype=jnp.int32)[None, None, :]).astype(jnp.int32)
    earlier_count = jnp.cumsum(onehot_rows, axis=1) - onehot_rows
    slot_index = lax.optimization_barrier(jnp.sum(earlier_count * onehot_rows, axis=2))
    column = (jnp.arange(N_EP, dtype=jnp.int32)[:, None] * CAP + slot_index).reshape(-1).astype(jnp.int32)
    flat_routes = routes.reshape(-1)
    token_index = jnp.repeat(jnp.arange(SEQS, dtype=jnp.int32), TOPK)
    slot_table = jnp.full((EXPERTS, N_EP * CAP), SEQS, jnp.int32).at[flat_routes, column].set(token_index)
    padded_rows = jnp.concatenate([hidden, jnp.zeros((1, D), jnp.bfloat16)], axis=0)

    def one_expert(packed):
        row_index, gate_mat, up_mat, down_mat = packed
        rows = padded_rows[row_index]
        gate_act = jnp.dot(rows, gate_mat, preferred_element_type=jnp.float32)
        up_act = jnp.dot(rows, up_mat, preferred_element_type=jnp.float32)
        inner = (jax.nn.silu(gate_act) * up_act).astype(jnp.bfloat16)
        return split_sum(inner, down_mat, N_TP).astype(jnp.bfloat16)
    results = lax.map(one_expert, (slot_table, expert_gate, expert_up, expert_down))
    picked = results[flat_routes, column].astype(jnp.float32).reshape(SEQS, TOPK, D)
    routed = lax.optimization_barrier(jnp.sum(route_weights[:, :, None] * picked, axis=1))
    shared_g = jnp.dot(hidden, shared_gate, preferred_element_type=jnp.float32)
    shared_u = jnp.dot(hidden, shared_up, preferred_element_type=jnp.float32)
    shared_inner = (jax.nn.silu(shared_g) * shared_u).astype(jnp.bfloat16)
    shared_result = split_sum(shared_inner, shared_down, N_TP)
    mixed_rows = RESIDUAL_SCALE * hidden.astype(jnp.float32) + routed + shared_result
    output = layer_norm(mixed_rows, final_gain).astype(jnp.bfloat16)
    return (output, new_keys, new_values)
```

```python
import functools

import jax
import jax.numpy as jnp
from jax import lax
from jax.experimental import pallas as pl
from jax.experimental.pallas import tpu as pltpu
from jax.sharding import PartitionSpec as P

RESIDUAL_SCALE = 2.0**0.25
ROUTE_SCALE = 2.5
NORM_EPS = 1e-05
F32 = jnp.float32
BF16 = jnp.bfloat16
VMEM = pltpu.VMEM
SEQ_STEP = 8
CUM = 256
AHEAD = 3


def iota(shape, dim):
    return lax.broadcasted_iota(jnp.int32, shape, dim)


def dot(a, b):
    return jnp.dot(a, b, preferred_element_type=F32)


def dot_nt(a, b):
    return lax.dot_general(a, b, (((1,), (1,)), ((), ())), preferred_element_type=F32)


def whole():
    return pl.BlockSpec(memory_space=VMEM)


def in_hbm(*arrays):
    return [pltpu.with_memory_space_constraint(x, pltpu.HBM) for x in arrays]


def swapped(x):
    return lax.ppermute(x, "tp", [(0, 1), (1, 0)])


def attend_kernel(
    len_hbm, bias_hbm, x_hbm, wq_hbm, k_hbm, v_hbm, wo_hbm, o_ref,
    len_scr, bias_scr, x_scr, wq_scr, k_scr, v_scr, wo_scr, q_scr, at_scr, tri_scr,
    sems, k_sems, v_sems,
):
    seqs, size, length = k_scr.shape
    heads = bias_scr.shape[0]
    blocks = length // CUM
    steps = seqs // SEQ_STEP
    small = [
        pltpu.make_async_copy(src, dst, sems.at[i])
        for i, (src, dst) in enumerate(
            [(x_hbm, x_scr), (wq_hbm, wq_scr), (len_hbm, len_scr), (bias_hbm, bias_scr)]
        )
    ]
    wo_copy = pltpu.make_async_copy(wo_hbm, wo_scr, sems.at[4])

    def cache_copies(step):
        part = pl.ds(step * SEQ_STEP, SEQ_STEP)
        return (
            pltpu.make_async_copy(k_hbm.at[part], k_scr.at[part], k_sems.at[step]),
            pltpu.make_async_copy(v_hbm.at[part], v_scr.at[part], v_sems.at[step]),
        )

    for copy in small:
        copy.start()
    for step in range(AHEAD):
        for copy in cache_copies(step):
            copy.start()
    row, col = iota((CUM, CUM), 0), iota((CUM, CUM), 1)
    tri_scr[...] = jnp.where(row > col, 1.0, 0.0).astype(BF16)
    for copy in small:
        copy.wait()
    query = dot(x_scr[...], wq_scr[...]).astype(BF16).astype(F32) * size**-0.5
    for g in range(heads):
        q_scr[pl.ds(g, seqs, stride=heads), :] = query[:, g * size : (g + 1) * size]
    head = iota((heads, 1), 0)
    bias = jnp.zeros((heads, 1), F32)
    for g in range(heads):
        bias = jnp.where(head == g, bias_scr[g], bias)
    position = iota((heads, length), 1)

    def one_step(step, carry):
        k_copy, v_copy = cache_copies(step)

        @pl.when(step + AHEAD < steps)
        def _():
            for copy in cache_copies(step + AHEAD):
                copy.start()

        @pl.when(step + AHEAD == steps)
        def _():
            wo_copy.start()

        k_copy.wait()
        scores, usable, soft = [], [], []
        for i in range(SEQ_STEP):
            seq = step * SEQ_STEP + i
            query = q_scr[pl.ds(pl.multiple_of(seq * heads, heads), heads), :]
            x = dot(query.astype(BF16), k_scr[seq]) + bias
            ok = position < len_scr[seq]
            sp = jnp.maximum(x, 0.0) + jnp.log(1.0 + jnp.exp(-jnp.abs(x)))
            scores.append(x - sp)
            usable.append(ok)
            soft.append(jnp.where(ok, sp, 0.0).astype(BF16))
        stacked = jnp.concatenate(
            [s[:, b * CUM : (b + 1) * CUM] for s in soft for b in range(blocks)], axis=0
        )
        sums = dot(stacked, tri_scr[...])
        totals = sums[:, :1] + stacked[:, :1].astype(F32)
        v_copy.wait()
        for i in range(SEQ_STEP):
            base = i * blocks * heads
            after = jnp.zeros((heads, 1), F32)
            parts = [None] * blocks
            for b in reversed(range(blocks)):
                rows = slice(base + b * heads, base + (b + 1) * heads)
                parts[b] = sums[rows, :] + after
                after = after + totals[rows]
            later = jnp.concatenate(parts, axis=1)
            weight = jnp.where(usable[i], jnp.exp(scores[i] - later), 0.0).astype(BF16)
            seq = step * SEQ_STEP + i
            at_scr[pl.ds(pl.multiple_of(seq * heads, heads), heads), :] = dot_nt(weight, v_scr[seq])
        return carry

    lax.fori_loop(0, steps, one_step, 0)
    attended = jnp.concatenate(
        [at_scr[pl.ds(g, seqs, stride=heads), :] for g in range(heads)], axis=1
    ).astype(BF16)
    wo_copy.wait()
    o_ref[...] = dot(attended, wo_scr[...]).astype(BF16)


def attend(inputs, keys, values, lengths, wq, head_bias, wo):
    seqs, width = inputs.shape
    size, length = keys.shape[1:]
    heads = head_bias.shape[0]
    steps = seqs // SEQ_STEP
    return pl.pallas_call(
        attend_kernel,
        out_shape=jax.ShapeDtypeStruct((seqs, width), BF16),
        in_specs=[pl.BlockSpec(memory_space=pl.ANY)] * 7,
        out_specs=whole(),
        scratch_shapes=[
            pltpu.SMEM((seqs,), jnp.int32),
            pltpu.SMEM((heads,), F32),
            VMEM(inputs.shape, BF16),
            VMEM(wq.shape, BF16),
            VMEM(keys.shape, BF16),
            VMEM(values.shape, BF16),
            VMEM(wo.shape, BF16),
            VMEM((seqs * heads, size), F32),
            VMEM((seqs * heads, size), F32),
            VMEM((CUM, CUM), BF16),
            pltpu.SemaphoreType.DMA((5,)),
            pltpu.SemaphoreType.DMA((steps,)),
            pltpu.SemaphoreType.DMA((steps,)),
        ],
        compiler_params=pltpu.CompilerParams(vmem_limit_bytes=36 * 2**20),
        cost_estimate=pl.CostEstimate(
            flops=8 * 10**9, bytes_accessed=22 * 10**6, transcendentals=2 * 10**6
        ),
        name="attend",
    )(*in_hbm(lengths, head_bias, inputs, wq, keys, values, wo))


def place_kernel(core_ref, routes_ref, place_ref, member_ref):
    choices, lanes = routes_ref.shape
    experts = member_ref.shape[0]
    rows = place_ref.shape[0]
    half = lanes // 2
    slots = rows // experts // 2
    expert = iota((experts, lanes), 0)
    named = expert == routes_ref[0:1, :]
    for k in range(1, choices):
        named = named | (expert == routes_ref[k : k + 1, :])
    member = jnp.where(named, 1.0, 0.0)
    member_ref[...] = member
    a, b = iota((lanes, lanes), 0), iota((lanes, lanes), 1)
    earlier = jnp.where((a < b) & ((a < half) == (b < half)), 1.0, 0.0).astype(BF16)
    slot = dot(member.astype(BF16), earlier)
    code = ((slot + 1.0) * member).astype(BF16)
    r, e = iota((rows, experts), 0), iota((rows, experts), 1)
    spread = jnp.where(r // (2 * slots) == e, 1.0, 0.0).astype(BF16)
    found = dot(spread, code)
    r, lane = iota((rows, lanes), 0), iota((rows, lanes), 1)
    wanted = (r % slots + 1 + core_ref[0] * slots).astype(F32)
    same_half = ((r // slots) % 2 == 0) == (lane < half)
    place_ref[...] = jnp.where((found == wanted) & same_half, 1.0, 0.0).astype(BF16)


def place(core, routes2, experts, slots):
    lanes = routes2.shape[1]
    return pl.pallas_call(
        place_kernel,
        out_shape=(
            jax.ShapeDtypeStruct((experts * 2 * slots, lanes), BF16),
            jax.ShapeDtypeStruct((experts, lanes), F32),
        ),
        in_specs=[pl.BlockSpec(memory_space=pltpu.SMEM), whole()],
        out_specs=(whole(), whole()),
        compiler_params=pltpu.CompilerParams(vmem_limit_bytes=8 * 2**20),
        cost_estimate=pl.CostEstimate(flops=10**8, bytes_accessed=10**5, transcendentals=0),
        name="place",
    )(core, routes2)


def halves(x):
    half = x.shape[1] // 2
    return jnp.concatenate([x[:, :half], x[:, half:]], axis=0)


def dispatch_kernel(
    x_ref, own_ref, other_ref, gain_ref, place_ref, hidden_hbm, out_ref, hidden_scr, sem
):
    v = (
        RESIDUAL_SCALE * x_ref[...].astype(F32)
        + own_ref[...].astype(F32)
        + other_ref[...].astype(F32)
    )
    centered = v - jnp.mean(v, axis=1, keepdims=True)
    var = jnp.mean(centered * centered, axis=1, keepdims=True)
    hidden = (centered * lax.rsqrt(var + NORM_EPS) * gain_ref[...]).astype(BF16)
    hidden_scr[...] = hidden
    copy = pltpu.make_async_copy(hidden_scr, hidden_hbm, sem)
    copy.start()
    out_ref[...] = dot(place_ref[...], halves(hidden)).astype(BF16)
    copy.wait()


def dispatch(inputs, own, other, gain, placement):
    seqs, width = inputs.shape
    return pl.pallas_call(
        dispatch_kernel,
        out_shape=(
            pltpu.HBM((seqs, width), BF16),
            jax.ShapeDtypeStruct((placement.shape[0], width // 2), BF16),
        ),
        in_specs=[whole()] * 5,
        out_specs=(pl.BlockSpec(memory_space=pltpu.HBM), whole()),
        scratch_shapes=[VMEM((seqs, width), BF16), pltpu.SemaphoreType.DMA],
        compiler_params=pltpu.CompilerParams(vmem_limit_bytes=12 * 2**20),
        cost_estimate=pl.CostEstimate(flops=2 * 10**8, bytes_accessed=2 * 10**6, transcendentals=64),
        name="dispatch",
    )(inputs, own, other, gain.reshape(1, width), placement)


def local_kernel(
    hidden_ref, x_ref, router_ref, member_ref, place_ref, sg_ref, su_ref, sd_ref, wk_ref, wv_ref,
    shared_ref, weight_ref, nk_ref, nv_ref,
):
    hidden = hidden_ref[...]
    gate, up = dot(hidden, sg_ref[...]), dot(hidden, su_ref[...])
    inner = (gate / (1.0 + jnp.exp(-gate)) * up).astype(BF16)
    shared_ref[...] = dot(inner, sd_ref[...])
    probs = 1.0 / (1.0 + jnp.exp(-dot_nt(router_ref[...], hidden)))
    probs = jnp.concatenate([probs, probs], axis=1) * member_ref[...]
    weights = ROUTE_SCALE * probs / jnp.sum(probs, axis=0, keepdims=True)
    experts = weights.shape[0]
    rows, lanes = place_ref.shape
    r, e = iota((rows, experts), 0), iota((rows, experts), 1)
    spread = jnp.where(r // (rows // experts) == e, 1.0, 0.0)
    placed = jnp.dot(spread, weights, precision=lax.Precision.HIGHEST, preferred_element_type=F32)
    placed = (placed * place_ref[...].astype(F32)).T
    high = placed.astype(BF16)
    weight_ref[:lanes, :] = high
    weight_ref[lanes:, :] = (placed - high.astype(F32)).astype(BF16)
    x = x_ref[...]
    nk_ref[...] = dot_nt(x, wk_ref[...]).astype(BF16)
    nv_ref[...] = dot_nt(x, wv_ref[...]).astype(BF16)


def local(hidden, inputs, router_t, member, placement, sg, su, sd, wk_t, wv_t):
    seqs, width = hidden.shape
    rows, lanes = placement.shape
    size = wk_t.shape[0]
    return pl.pallas_call(
        local_kernel,
        out_shape=(
            jax.ShapeDtypeStruct((seqs, width), F32),
            jax.ShapeDtypeStruct((2 * lanes, rows), BF16),
            jax.ShapeDtypeStruct((seqs, size), BF16),
            jax.ShapeDtypeStruct((seqs, size), BF16),
        ),
        in_specs=[whole()] * 10,
        out_specs=(whole(),) * 4,
        compiler_params=pltpu.CompilerParams(vmem_limit_bytes=20 * 2**20),
        cost_estimate=pl.CostEstimate(
            flops=4 * 10**9, bytes_accessed=5 * 10**6, transcendentals=10**5
        ),
        name="local",
    )(hidden, inputs, router_t, member, placement, *in_hbm(sg, su, sd, wk_t, wv_t))


def expert_kernel(order_ref, rows_ref, *refs):
    weights, out_ref = refs[:-1], refs[-1]
    groups, lines, half = rows_ref.shape
    slots = lines // 2
    low = iota((groups // 2, lines, half), 1) < slots
    x = rows_ref[...].astype(F32).reshape(groups // 2, 2, lines, half)
    a, b = x[:, 0], x[:, 1]
    count = groups * slots
    first = jnp.where(low, a, pltpu.roll(b, slots, 1)).reshape(count, half).astype(BF16)
    second = jnp.where(low, pltpu.roll(a, slots, 1), b).reshape(count, half).astype(BF16)
    total = None
    for i in range(2):
        gate_ref, up_ref, down_ref = weights[3 * i : 3 * i + 3]
        gate = dot(first, gate_ref[:half, :]) + dot(second, gate_ref[half:, :])
        up = dot(first, up_ref[:half, :]) + dot(second, up_ref[half:, :])
        inner = (gate / (1.0 + jnp.exp(-gate)) * up).astype(BF16)
        part = dot(inner, down_ref[...]).astype(BF16).astype(F32)
        total = part if total is None else total + part
    a = total[:, :half].reshape(groups // 2, lines, half)
    b = total[:, half:].reshape(groups // 2, lines, half)
    even = jnp.where(low, a, pltpu.roll(b, slots, 1))
    odd = jnp.where(low, pltpu.roll(a, slots, 1), b)
    out_ref[...] = jnp.stack([even, odd], axis=1).reshape(groups, lines, half).astype(BF16)


def expert(order, rows, weights):
    return pl.pallas_call(
        expert_kernel,
        out_shape=jax.ShapeDtypeStruct(rows.shape, BF16),
        in_specs=[pl.BlockSpec(memory_space=pl.ANY)] + [whole()] * 7,
        out_specs=whole(),
        compiler_params=pltpu.CompilerParams(vmem_limit_bytes=32 * 2**20),
        cost_estimate=pl.CostEstimate(
            flops=2 * 10**9, bytes_accessed=8 * 10**6, transcendentals=3 * 10**5
        ),
        name="expert",
    )(*in_hbm(order), rows, *weights)


def combine_kernel(weight_ref, rows_ref, shared_ref, mine_ref, send_ref):
    lanes = weight_ref.shape[0] // 2
    both = dot(weight_ref[...], rows_ref[...])
    part = both[:lanes, :] + both[lanes:, :] + halves(shared_ref[...])
    mine_ref[...] = part
    send_ref[...] = part.astype(BF16)


def combine(weight, rows, shared):
    shape = (weight.shape[0] // 2, rows.shape[1])
    return pl.pallas_call(
        combine_kernel,
        out_shape=(jax.ShapeDtypeStruct(shape, F32), jax.ShapeDtypeStruct(shape, BF16)),
        in_specs=[whole()] * 3,
        out_specs=(whole(), whole()),
        compiler_params=pltpu.CompilerParams(vmem_limit_bytes=16 * 2**20),
        cost_estimate=pl.CostEstimate(flops=3 * 10**8, bytes_accessed=3 * 10**6, transcendentals=0),
        name="combine",
    )(weight, rows, shared)


def finish_kernel(core_ref, mine_ref, other_ref, hidden_ref, gain_ref, out_ref, mixed):
    seqs, half = out_ref.shape
    v = mine_ref[...] + other_ref[...].astype(F32) + RESIDUAL_SCALE * halves(hidden_ref[...]).astype(F32)
    mixed[...] = v
    sums = jnp.sum(v, axis=1, keepdims=True)
    mean = (sums[:seqs] + sums[seqs:]) / (2 * half)
    centered = v - jnp.concatenate([mean, mean], axis=0)
    squares = jnp.sum(centered * centered, axis=1, keepdims=True)
    scale = lax.rsqrt((squares[:seqs] + squares[seqs:]) / (2 * half) + NORM_EPS)
    own = mixed[pl.ds(pl.multiple_of(core_ref[0] * seqs, seqs), seqs), :]
    out_ref[...] = ((own - mean) * scale * gain_ref[...]).astype(BF16)


def finish(core, mine, other, hidden, gain):
    lanes, half = mine.shape
    return pl.pallas_call(
        finish_kernel,
        out_shape=jax.ShapeDtypeStruct((lanes // 2, half), BF16),
        in_specs=[pl.BlockSpec(memory_space=pltpu.SMEM)] + [whole()] * 4,
        out_specs=whole(),
        scratch_shapes=[VMEM((lanes, half), F32)],
        compiler_params=pltpu.CompilerParams(vmem_limit_bytes=12 * 2**20),
        cost_estimate=pl.CostEstimate(flops=10**7, bytes_accessed=2 * 10**6, transcendentals=64),
        name="finish",
    )(core, mine, other, hidden, gain.reshape(1, half))


def on_device(
    inputs,
    cache_keys,
    cache_values,
    lengths,
    query_weight,
    key_weight,
    value_weight,
    head_bias,
    out_weight,
    attend_gain,
    router_weight,
    routes,
    expert_gate,
    expert_up,
    expert_down,
    shared_gate,
    shared_up,
    shared_down,
    final_gain,
):
    seqs, width = inputs.shape
    experts = router_weight.shape[1]
    slots = 2 * seqs * routes.shape[1] // experts // 2
    core = lax.axis_index("tp").astype(jnp.int32).reshape(1)
    own_part = attend(
        inputs, cache_keys[:, 0], cache_values[:, 0], lengths, query_weight, head_bias, out_weight
    )
    other_part = swapped(own_part)
    routes_t = routes.T
    placement, member = place(core, jnp.concatenate([routes_t, routes_t], axis=1), experts, slots)
    hidden, outgoing = dispatch(inputs, own_part, other_part, attend_gain, placement)
    arrived = lax.all_to_all(
        outgoing.reshape(experts, 2 * slots, width // 2), "ep", 0, 0, tiled=True
    )
    own_weights = (expert_gate[0], expert_up[0], expert_down[0])
    other_weights = tuple(swapped(w) for w in own_weights)
    shared, weight, new_keys, new_values = local(
        hidden, inputs, router_weight.T, member, placement, shared_gate, shared_up, shared_down,
        key_weight.T, value_weight.T,
    )
    results = expert(new_keys, arrived, own_weights + other_weights)
    returned = lax.all_to_all(results, "ep", 0, 0, tiled=True)
    mine, send = combine(weight, returned.reshape(experts * 2 * slots, width // 2), shared)
    output = finish(core, mine, swapped(send), hidden, final_gain)
    return (output, new_keys, new_values)


def solution(mesh):
    placed = (
        P("ep", None),
        P("ep", "tp", None, None),
        P("ep", "tp", None, None),
        P("ep"),
        P(None, "tp"),
        P(None, "tp"),
        P(None, "tp"),
        P("tp"),
        P("tp", None),
        P(),
        P(),
        P("ep", None),
        P("ep", None, "tp"),
        P("ep", None, "tp"),
        P("ep", "tp", None),
        P(None, "tp"),
        P(None, "tp"),
        P("tp", None),
        P("tp"),
    )
    return jax.shard_map(
        on_device,
        mesh=mesh,
        in_specs=placed,
        out_specs=(P("ep", "tp"), P("ep", "tp"), P("ep", "tp")),
        check_vma=False,
    )
```

```python
import functools

import jax
import jax.numpy as jnp
from jax import lax
from jax.experimental import pallas as pl
from jax.experimental.pallas import tpu as pltpu
from jax.sharding import PartitionSpec as P

RESIDUAL_SCALE = 2.0**0.25
ROUTE_SCALE = 2.5
NORM_EPS = 1e-05
F32 = jnp.float32
BF16 = jnp.bfloat16
VMEM = pltpu.VMEM
SEQ_STEP = 16
CUM = 256
COLUMNS = 256
PIECES = 4
AHEAD = 2


def iota(shape, dim):
    return lax.broadcasted_iota(jnp.int32, shape, dim)


def dot(a, b):
    return jnp.dot(a, b, preferred_element_type=F32)


def dot_nt(a, b):
    return lax.dot_general(a, b, (((1,), (1,)), ((), ())), preferred_element_type=F32)


def whole():
    return pl.BlockSpec(memory_space=VMEM)


def in_hbm(*arrays):
    return [pltpu.with_memory_space_constraint(x, pltpu.HBM) for x in arrays]


def swapped(x):
    return lax.ppermute(x, "tp", [(0, 1), (1, 0)])


def attend_kernel(
    len_hbm, bias_hbm, x_hbm, wq_hbm, k_hbm, v_hbm, wo_hbm, o_ref,
    len_scr, bias_scr, x_scr, wq_scr, k_scr, v_scr, wo_scr, q_scr, at_scr, tri_scr,
    sems, k_sems, v_sems,
):
    seqs, size, length = k_scr.shape
    heads = bias_scr.shape[0]
    blocks = length // CUM
    steps = seqs // SEQ_STEP
    small = [
        pltpu.make_async_copy(src, dst, sems.at[i])
        for i, (src, dst) in enumerate(
            [(x_hbm, x_scr), (wq_hbm, wq_scr), (len_hbm, len_scr), (bias_hbm, bias_scr)]
        )
    ]
    wo_copy = pltpu.make_async_copy(wo_hbm, wo_scr, sems.at[4])

    def cache_copies(step):
        part = pl.ds(step * SEQ_STEP, SEQ_STEP)
        return (
            pltpu.make_async_copy(k_hbm.at[part], k_scr.at[part], k_sems.at[step]),
            pltpu.make_async_copy(v_hbm.at[part], v_scr.at[part], v_sems.at[step]),
        )

    for copy in small:
        copy.start()
    for step in range(AHEAD):
        for copy in cache_copies(step):
            copy.start()
    row, col = iota((CUM, CUM), 0), iota((CUM, CUM), 1)
    tri_scr[...] = jnp.where(row > col, 1.0, 0.0).astype(BF16)
    for copy in small:
        copy.wait()
    query = dot(x_scr[...], wq_scr[...]).astype(BF16).astype(F32) * size**-0.5
    for g in range(heads):
        q_scr[pl.ds(g, seqs, stride=heads), :] = query[:, g * size : (g + 1) * size]
    head = iota((heads, 1), 0)
    bias = jnp.zeros((heads, 1), F32)
    for g in range(heads):
        bias = jnp.where(head == g, bias_scr[g], bias)
    position = iota((heads, length), 1)

    def one_step(step, carry):
        k_copy, v_copy = cache_copies(step)

        @pl.when(step + AHEAD < steps)
        def _():
            for copy in cache_copies(step + AHEAD):
                copy.start()

        @pl.when(step + AHEAD == steps)
        def _():
            wo_copy.start()

        k_copy.wait()
        scores, usable, soft = [], [], []
        for i in range(SEQ_STEP):
            seq = step * SEQ_STEP + i
            query = q_scr[pl.ds(pl.multiple_of(seq * heads, heads), heads), :]
            x = dot(query.astype(BF16), k_scr[seq]) + bias
            ok = position < len_scr[seq]
            sp = jnp.maximum(x, 0.0) + jnp.log(1.0 + jnp.exp(-jnp.abs(x)))
            scores.append(x - sp)
            usable.append(ok)
            soft.append(jnp.where(ok, sp, 0.0).astype(BF16))
        stacked = jnp.concatenate(
            [s[:, b * CUM : (b + 1) * CUM] for s in soft for b in range(blocks)], axis=0
        )
        sums = dot(stacked, tri_scr[...])
        totals = sums[:, :1] + stacked[:, :1].astype(F32)
        v_copy.wait()
        for i in range(SEQ_STEP):
            base = i * blocks * heads
            after = jnp.zeros((heads, 1), F32)
            parts = [None] * blocks
            for b in reversed(range(blocks)):
                rows = slice(base + b * heads, base + (b + 1) * heads)
                parts[b] = sums[rows, :] + after
                after = after + totals[rows]
            later = jnp.concatenate(parts, axis=1)
            weight = jnp.where(usable[i], jnp.exp(scores[i] - later), 0.0).astype(BF16)
            seq = step * SEQ_STEP + i
            at_scr[pl.ds(pl.multiple_of(seq * heads, heads), heads), :] = dot_nt(weight, v_scr[seq])
        return carry

    lax.fori_loop(0, steps, one_step, 0)
    attended = jnp.concatenate(
        [at_scr[pl.ds(g, seqs, stride=heads), :] for g in range(heads)], axis=1
    ).astype(BF16)
    wo_copy.wait()
    o_ref[...] = dot(attended, wo_scr[...]).astype(BF16)


def attend(inputs, keys, values, lengths, wq, head_bias, wo):
    seqs, width = inputs.shape
    size, length = keys.shape[1:]
    heads = head_bias.shape[0]
    steps = seqs // SEQ_STEP
    return pl.pallas_call(
        attend_kernel,
        out_shape=jax.ShapeDtypeStruct((seqs, width), BF16),
        in_specs=[pl.BlockSpec(memory_space=pl.ANY)] * 7,
        out_specs=whole(),
        scratch_shapes=[
            pltpu.SMEM((seqs,), jnp.int32),
            pltpu.SMEM((heads,), F32),
            VMEM(inputs.shape, BF16),
            VMEM(wq.shape, BF16),
            VMEM(keys.shape, BF16),
            VMEM(values.shape, BF16),
            VMEM(wo.shape, BF16),
            VMEM((seqs * heads, size), F32),
            VMEM((seqs * heads, size), F32),
            VMEM((CUM, CUM), BF16),
            pltpu.SemaphoreType.DMA((5,)),
            pltpu.SemaphoreType.DMA((steps,)),
            pltpu.SemaphoreType.DMA((steps,)),
        ],
        compiler_params=pltpu.CompilerParams(vmem_limit_bytes=36 * 2**20),
        cost_estimate=pl.CostEstimate(
            flops=8 * 10**9, bytes_accessed=22 * 10**6, transcendentals=2 * 10**6
        ),
        name="attend",
    )(*in_hbm(lengths, head_bias, inputs, wq, keys, values, wo))


def place_kernel(core_ref, routes_ref, place_ref, member_ref):
    choices, lanes = routes_ref.shape
    experts = member_ref.shape[0]
    rows = place_ref.shape[0]
    half = lanes // 2
    slots = rows // experts // 2
    expert = iota((experts, lanes), 0)
    named = expert == routes_ref[0:1, :]
    for k in range(1, choices):
        named = named | (expert == routes_ref[k : k + 1, :])
    member = jnp.where(named, 1.0, 0.0)
    member_ref[...] = member
    a, b = iota((lanes, lanes), 0), iota((lanes, lanes), 1)
    earlier = jnp.where((a < b) & ((a < half) == (b < half)), 1.0, 0.0).astype(BF16)
    slot = dot(member.astype(BF16), earlier)
    code = ((slot + 1.0) * member).astype(BF16)
    r, e = iota((rows, experts), 0), iota((rows, experts), 1)
    spread = jnp.where(r // (2 * slots) == e, 1.0, 0.0).astype(BF16)
    found = dot(spread, code)
    r, lane = iota((rows, lanes), 0), iota((rows, lanes), 1)
    wanted = (r % slots + 1 + core_ref[0] * slots).astype(F32)
    same_half = ((r // slots) % 2 == 0) == (lane < half)
    place_ref[...] = jnp.where((found == wanted) & same_half, 1.0, 0.0).astype(BF16)


def place(core, routes2, experts, slots):
    lanes = routes2.shape[1]
    return pl.pallas_call(
        place_kernel,
        out_shape=(
            jax.ShapeDtypeStruct((experts * 2 * slots, lanes), BF16),
            jax.ShapeDtypeStruct((experts, lanes), F32),
        ),
        in_specs=[pl.BlockSpec(memory_space=pltpu.SMEM), whole()],
        out_specs=(whole(), whole()),
        compiler_params=pltpu.CompilerParams(vmem_limit_bytes=8 * 2**20),
        cost_estimate=pl.CostEstimate(flops=10**8, bytes_accessed=10**5, transcendentals=0),
        name="place",
    )(core, routes2)


def halves(x):
    half = x.shape[1] // 2
    return jnp.concatenate([x[:, :half], x[:, half:]], axis=0)


def dispatch_kernel(
    x_ref, own_ref, other_ref, gain_ref, place_ref, hidden_hbm, out_hbm, hidden_scr, out_scr, sems
):
    v = (
        RESIDUAL_SCALE * x_ref[...].astype(F32)
        + own_ref[...].astype(F32)
        + other_ref[...].astype(F32)
    )
    centered = v - jnp.mean(v, axis=1, keepdims=True)
    var = jnp.mean(centered * centered, axis=1, keepdims=True)
    hidden = (centered * lax.rsqrt(var + NORM_EPS) * gain_ref[...]).astype(BF16)
    hidden_scr[...] = hidden
    copies = [pltpu.make_async_copy(hidden_scr, hidden_hbm, sems.at[PIECES])]
    stacked = halves(hidden)
    rows = out_scr.shape[0] // PIECES
    for i in range(PIECES):
        part = pl.ds(i * rows, rows)
        out_scr[part, :] = dot(place_ref[part, :], stacked).astype(BF16)
        copies.append(pltpu.make_async_copy(out_scr.at[part], out_hbm.at[part], sems.at[i]))
        copies[-1].start()
    copies[0].start()
    for copy in copies:
        copy.wait()


def dispatch(inputs, own, other, gain, placement):
    seqs, width = inputs.shape
    return pl.pallas_call(
        dispatch_kernel,
        out_shape=(
            pltpu.HBM((seqs, width), BF16),
            pltpu.HBM((placement.shape[0], width // 2), BF16),
        ),
        in_specs=[whole()] * 5,
        out_specs=(pl.BlockSpec(memory_space=pltpu.HBM),) * 2,
        scratch_shapes=[
            VMEM((seqs, width), BF16),
            VMEM((placement.shape[0], width // 2), BF16),
            pltpu.SemaphoreType.DMA((PIECES + 1,)),
        ],
        compiler_params=pltpu.CompilerParams(vmem_limit_bytes=12 * 2**20),
        cost_estimate=pl.CostEstimate(flops=2 * 10**8, bytes_accessed=2 * 10**6, transcendentals=64),
        name="dispatch",
    )(inputs, own, other, gain.reshape(1, width), placement)


def local_kernel(
    hidden_hbm, x_hbm, router_hbm, member_ref, place_ref, sg_hbm, su_hbm, sd_hbm, wk_hbm, wv_hbm,
    shared_ref, weight_ref, nk_ref, nv_ref, *scratch,
):
    *buffers, sems = scratch
    sources = [hidden_hbm, sg_hbm, su_hbm, sd_hbm, router_hbm, x_hbm, wk_hbm, wv_hbm]
    copies = [
        pltpu.make_async_copy(src, dst, sems.at[i])
        for i, (src, dst) in enumerate(zip(sources, buffers))
    ]
    for copy in copies:
        copy.start()
    hidden_ref, sg_ref, su_ref, sd_ref, router_ref, x_ref, wk_ref, wv_ref = buffers
    for copy in copies[:3]:
        copy.wait()
    hidden = hidden_ref[...]
    gate, up = dot(hidden, sg_ref[...]), dot(hidden, su_ref[...])
    inner = (gate / (1.0 + jnp.exp(-gate)) * up).astype(BF16)
    for copy in copies[3:]:
        copy.wait()
    shared_ref[...] = dot(inner, sd_ref[...])
    probs = 1.0 / (1.0 + jnp.exp(-dot_nt(router_ref[...], hidden)))
    probs = jnp.concatenate([probs, probs], axis=1) * member_ref[...]
    weights = ROUTE_SCALE * probs / jnp.sum(probs, axis=0, keepdims=True)
    experts = weights.shape[0]
    rows, lanes = place_ref.shape
    r, e = iota((rows, experts), 0), iota((rows, experts), 1)
    spread = jnp.where(r // (rows // experts) == e, 1.0, 0.0)
    placed = jnp.dot(spread, weights, precision=lax.Precision.HIGHEST, preferred_element_type=F32)
    placed = (placed * place_ref[...].astype(F32)).T
    high = placed.astype(BF16)
    weight_ref[:lanes, :] = high
    weight_ref[lanes:, :] = (placed - high.astype(F32)).astype(BF16)
    x = x_ref[...]
    nk_ref[...] = dot_nt(x, wk_ref[...]).astype(BF16)
    nv_ref[...] = dot_nt(x, wv_ref[...]).astype(BF16)


def local(hidden, inputs, router_t, member, placement, sg, su, sd, wk_t, wv_t):
    seqs, width = hidden.shape
    rows, lanes = placement.shape
    size = wk_t.shape[0]
    any_space = pl.BlockSpec(memory_space=pl.ANY)
    buffered = [hidden, sg, su, sd, router_t, inputs, wk_t, wv_t]
    return pl.pallas_call(
        local_kernel,
        out_shape=(
            jax.ShapeDtypeStruct((seqs, width), F32),
            jax.ShapeDtypeStruct((2 * lanes, rows), BF16),
            jax.ShapeDtypeStruct((seqs, size), BF16),
            jax.ShapeDtypeStruct((seqs, size), BF16),
        ),
        in_specs=[any_space] * 3 + [whole()] * 2 + [any_space] * 5,
        out_specs=(whole(),) * 4,
        scratch_shapes=[VMEM(b.shape, b.dtype) for b in buffered]
        + [pltpu.SemaphoreType.DMA((len(buffered),))],
        compiler_params=pltpu.CompilerParams(vmem_limit_bytes=24 * 2**20),
        cost_estimate=pl.CostEstimate(
            flops=4 * 10**9, bytes_accessed=5 * 10**6, transcendentals=10**5
        ),
        name="local",
    )(
        *in_hbm(hidden, inputs, router_t), member, placement, *in_hbm(sg, su, sd, wk_t, wv_t)
    )


def expert_kernel(
    order_ref, rows_ref, own_gate_ref, own_up_ref, down_hbm, gate2_hbm, up2_hbm, down2_hbm, out_ref,
    down_scr, gate2_scr, up2_scr, down2_scr, sems,
):
    sources = [gate2_hbm, up2_hbm, down_hbm, down2_hbm]
    buffers = [gate2_scr, up2_scr, down_scr, down2_scr]
    gate_copy, up_copy, *down_copies = [
        pltpu.make_async_copy(src, dst, sems.at[i])
        for i, (src, dst) in enumerate(zip(sources, buffers))
    ]
    gate_copy.start()
    up_copy.start()
    groups, lines, half = rows_ref.shape
    slots = lines // 2
    low = iota((groups // 2, lines, half), 1) < slots
    x = rows_ref[...].astype(F32).reshape(groups // 2, 2, lines, half)
    a, b = x[:, 0], x[:, 1]
    count = groups * slots
    first = jnp.where(low, a, pltpu.roll(b, slots, 1)).reshape(count, half).astype(BF16)
    second = jnp.where(low, pltpu.roll(a, slots, 1), b).reshape(count, half).astype(BF16)

    def product(ref):
        return dot(first, ref[:half, :]) + dot(second, ref[half:, :])

    def gated(gate, up):
        return (gate / (1.0 + jnp.exp(-gate)) * up).astype(BF16)

    gate, up = product(own_gate_ref), product(own_up_ref)
    for copy in down_copies:
        copy.start()
    own = gated(gate, up)
    gate_copy.wait()
    up_copy.wait()
    other = gated(product(gate2_scr), product(up2_scr))
    for copy in down_copies:
        copy.wait()

    def result(start):
        cols = slice(start, start + COLUMNS)
        parts = [
            dot(inner, ref[:, cols]).astype(BF16).astype(F32)
            for inner, ref in ((own, down_scr), (other, down2_scr))
        ]
        return (parts[0] + parts[1]).reshape(groups // 2, lines, COLUMNS)

    low = iota((groups // 2, lines, COLUMNS), 1) < slots
    for start in range(0, half, COLUMNS):
        a, b = result(start), result(half + start)
        even = jnp.where(low, a, pltpu.roll(b, slots, 1))
        odd = jnp.where(low, pltpu.roll(a, slots, 1), b)
        both = jnp.stack([even, odd], axis=1).reshape(groups, lines, COLUMNS)
        out_ref[:, :, start : start + COLUMNS] = both.astype(BF16)


def expert(order, rows, weights):
    gate, up, *streamed = weights
    any_space = pl.BlockSpec(memory_space=pl.ANY)
    return pl.pallas_call(
        expert_kernel,
        out_shape=jax.ShapeDtypeStruct(rows.shape, BF16),
        in_specs=[any_space] + [whole()] * 3 + [any_space] * 4,
        out_specs=whole(),
        scratch_shapes=[VMEM(w.shape, w.dtype) for w in streamed]
        + [pltpu.SemaphoreType.DMA((len(streamed),))],
        compiler_params=pltpu.CompilerParams(vmem_limit_bytes=32 * 2**20),
        cost_estimate=pl.CostEstimate(
            flops=2 * 10**9, bytes_accessed=8 * 10**6, transcendentals=3 * 10**5
        ),
        name="expert",
    )(*in_hbm(order), rows, gate, up, *in_hbm(*streamed))


def combine_kernel(weight_ref, rows_ref, shared_ref, mine_ref, send_ref):
    lanes = weight_ref.shape[0] // 2
    both = dot(weight_ref[...], rows_ref[...])
    part = both[:lanes, :] + both[lanes:, :] + halves(shared_ref[...])
    mine_ref[...] = part
    send_ref[...] = part.astype(BF16)


def combine(weight, rows, shared):
    shape = (weight.shape[0] // 2, rows.shape[1])
    return pl.pallas_call(
        combine_kernel,
        out_shape=(jax.ShapeDtypeStruct(shape, F32), jax.ShapeDtypeStruct(shape, BF16)),
        in_specs=[whole()] * 3,
        out_specs=(whole(), whole()),
        compiler_params=pltpu.CompilerParams(vmem_limit_bytes=16 * 2**20),
        cost_estimate=pl.CostEstimate(flops=3 * 10**8, bytes_accessed=3 * 10**6, transcendentals=0),
        name="combine",
    )(weight, rows, shared)


def finish_kernel(core_ref, mine_ref, other_ref, hidden_ref, gain_ref, out_ref, mixed):
    seqs, half = out_ref.shape
    v = mine_ref[...] + other_ref[...].astype(F32) + RESIDUAL_SCALE * halves(hidden_ref[...]).astype(F32)
    mixed[...] = v
    sums = jnp.sum(v, axis=1, keepdims=True)
    mean = (sums[:seqs] + sums[seqs:]) / (2 * half)
    centered = v - jnp.concatenate([mean, mean], axis=0)
    squares = jnp.sum(centered * centered, axis=1, keepdims=True)
    scale = lax.rsqrt((squares[:seqs] + squares[seqs:]) / (2 * half) + NORM_EPS)
    own = mixed[pl.ds(pl.multiple_of(core_ref[0] * seqs, seqs), seqs), :]
    out_ref[...] = ((own - mean) * scale * gain_ref[...]).astype(BF16)


def finish(core, mine, other, hidden, gain):
    lanes, half = mine.shape
    return pl.pallas_call(
        finish_kernel,
        out_shape=jax.ShapeDtypeStruct((lanes // 2, half), BF16),
        in_specs=[pl.BlockSpec(memory_space=pltpu.SMEM)] + [whole()] * 4,
        out_specs=whole(),
        scratch_shapes=[VMEM((lanes, half), F32)],
        compiler_params=pltpu.CompilerParams(vmem_limit_bytes=12 * 2**20),
        cost_estimate=pl.CostEstimate(flops=10**7, bytes_accessed=2 * 10**6, transcendentals=64),
        name="finish",
    )(core, mine, other, hidden, gain.reshape(1, half))


def on_device(
    inputs,
    cache_keys,
    cache_values,
    lengths,
    query_weight,
    key_weight,
    value_weight,
    head_bias,
    out_weight,
    attend_gain,
    router_weight,
    routes,
    expert_gate,
    expert_up,
    expert_down,
    shared_gate,
    shared_up,
    shared_down,
    final_gain,
):
    seqs, width = inputs.shape
    experts = router_weight.shape[1]
    slots = 2 * seqs * routes.shape[1] // experts // 2
    core = lax.axis_index("tp").astype(jnp.int32).reshape(1)
    own_part = attend(
        inputs, cache_keys[:, 0], cache_values[:, 0], lengths, query_weight, head_bias, out_weight
    )
    other_part = swapped(own_part)
    routes_t = routes.T
    placement, member = place(core, jnp.concatenate([routes_t, routes_t], axis=1), experts, slots)
    hidden, outgoing = dispatch(inputs, own_part, other_part, attend_gain, placement)
    arrived = lax.all_to_all(
        outgoing.reshape(experts, 2 * slots, width // 2), "ep", 0, 0, tiled=True
    )
    own_weights = (expert_gate[0], expert_up[0], expert_down[0])
    other_weights = tuple(swapped(w) for w in own_weights)
    shared, weight, new_keys, new_values = local(
        hidden, inputs, router_weight.T, member, placement, shared_gate, shared_up, shared_down,
        key_weight.T, value_weight.T,
    )
    results = expert(new_keys, arrived, own_weights + other_weights)
    returned = lax.all_to_all(results, "ep", 0, 0, tiled=True)
    mine, send = combine(weight, returned.reshape(experts * 2 * slots, width // 2), shared)
    output = finish(core, mine, swapped(send), hidden, final_gain)
    return (output, new_keys, new_values)


def solution(mesh):
    placed = (
        P("ep", None),
        P("ep", "tp", None, None),
        P("ep", "tp", None, None),
        P("ep"),
        P(None, "tp"),
        P(None, "tp"),
        P(None, "tp"),
        P("tp"),
        P("tp", None),
        P(),
        P(),
        P("ep", None),
        P("ep", None, "tp"),
        P("ep", None, "tp"),
        P("ep", "tp", None),
        P(None, "tp"),
        P(None, "tp"),
        P("tp", None),
        P("tp"),
    )
    return jax.shard_map(
        on_device,
        mesh=mesh,
        in_specs=placed,
        out_specs=(P("ep", "tp"), P("ep", "tp"), P("ep", "tp")),
        check_vma=False,
    )
```

```python
import functools

import jax
import jax.numpy as jnp
from jax import lax
from jax.experimental import pallas as pl
from jax.experimental.pallas import tpu as pltpu
from jax.sharding import PartitionSpec as P

RESIDUAL_SCALE = 2.0**0.25
ROUTE_SCALE = 2.5
NORM_EPS = 1e-05
F32 = jnp.float32
BF16 = jnp.bfloat16
VMEM = pltpu.VMEM
SEQ_STEP = 16
CUM = 256
COLUMNS = 256
PIECES = 4
AHEAD = 2


def iota(shape, dim):
    return lax.broadcasted_iota(jnp.int32, shape, dim)


def dot(a, b):
    return jnp.dot(a, b, preferred_element_type=F32)


def dot_nt(a, b):
    return lax.dot_general(a, b, (((1,), (1,)), ((), ())), preferred_element_type=F32)


def whole():
    return pl.BlockSpec(memory_space=VMEM)


def in_hbm(*arrays):
    return [pltpu.with_memory_space_constraint(x, pltpu.HBM) for x in arrays]


def swapped(x):
    return lax.ppermute(x, "tp", [(0, 1), (1, 0)])


def attend_kernel(
    len_hbm, bias_hbm, x_hbm, wq_hbm, k_hbm, v_hbm, wo_hbm, o_ref,
    len_scr, bias_scr, x_scr, wq_scr, k_scr, v_scr, wo_scr, q_scr, at_scr, tri_scr,
    sems, k_sems, v_sems,
):
    seqs, size, length = k_scr.shape
    heads = bias_scr.shape[0]
    blocks = length // CUM
    steps = seqs // SEQ_STEP
    small = [
        pltpu.make_async_copy(src, dst, sems.at[i])
        for i, (src, dst) in enumerate(
            [(x_hbm, x_scr), (wq_hbm, wq_scr), (len_hbm, len_scr), (bias_hbm, bias_scr)]
        )
    ]
    wo_copy = pltpu.make_async_copy(wo_hbm, wo_scr, sems.at[4])

    def cache_copies(step):
        part = pl.ds(step * SEQ_STEP, SEQ_STEP)
        return (
            pltpu.make_async_copy(k_hbm.at[part], k_scr.at[part], k_sems.at[step]),
            pltpu.make_async_copy(v_hbm.at[part], v_scr.at[part], v_sems.at[step]),
        )

    for copy in small:
        copy.start()
    for step in range(AHEAD):
        for copy in cache_copies(step):
            copy.start()
    row, col = iota((CUM, CUM), 0), iota((CUM, CUM), 1)
    tri_scr[...] = jnp.where(row > col, 1.0, 0.0).astype(BF16)
    for copy in small:
        copy.wait()
    query = dot(x_scr[...], wq_scr[...]).astype(BF16).astype(F32) * size**-0.5
    for g in range(heads):
        q_scr[pl.ds(g, seqs, stride=heads), :] = query[:, g * size : (g + 1) * size]
    head = iota((heads, 1), 0)
    bias = jnp.zeros((heads, 1), F32)
    for g in range(heads):
        bias = jnp.where(head == g, bias_scr[g], bias)
    position = iota((heads, length), 1)

    def one_step(step, carry):
        k_copy, v_copy = cache_copies(step)

        @pl.when(step + AHEAD < steps)
        def _():
            for copy in cache_copies(step + AHEAD):
                copy.start()

        @pl.when(step + AHEAD == steps)
        def _():
            wo_copy.start()

        k_copy.wait()
        scores, usable, soft = [], [], []
        for i in range(SEQ_STEP):
            seq = step * SEQ_STEP + i
            query = q_scr[pl.ds(pl.multiple_of(seq * heads, heads), heads), :]
            x = dot(query.astype(BF16), k_scr[seq]) + bias
            ok = position < len_scr[seq]
            sp = jnp.maximum(x, 0.0) + jnp.log(1.0 + jnp.exp(-jnp.abs(x)))
            scores.append(x - sp)
            usable.append(ok)
            soft.append(jnp.where(ok, sp, 0.0).astype(BF16))
        stacked = jnp.concatenate(
            [s[:, b * CUM : (b + 1) * CUM] for s in soft for b in range(blocks)], axis=0
        )
        sums = dot(stacked, tri_scr[...])
        totals = sums[:, :1] + stacked[:, :1].astype(F32)
        v_copy.wait()
        for i in range(SEQ_STEP):
            base = i * blocks * heads
            after = jnp.zeros((heads, 1), F32)
            parts = [None] * blocks
            for b in reversed(range(blocks)):
                rows = slice(base + b * heads, base + (b + 1) * heads)
                parts[b] = sums[rows, :] + after
                after = after + totals[rows]
            later = jnp.concatenate(parts, axis=1)
            weight = jnp.where(usable[i], jnp.exp(scores[i] - later), 0.0).astype(BF16)
            seq = step * SEQ_STEP + i
            at_scr[pl.ds(pl.multiple_of(seq * heads, heads), heads), :] = dot_nt(weight, v_scr[seq])
        return carry

    lax.fori_loop(0, steps, one_step, 0)
    attended = jnp.concatenate(
        [at_scr[pl.ds(g, seqs, stride=heads), :] for g in range(heads)], axis=1
    ).astype(BF16)
    wo_copy.wait()
    o_ref[...] = dot(attended, wo_scr[...]).astype(BF16)


def attend(inputs, keys, values, lengths, wq, head_bias, wo):
    seqs, width = inputs.shape
    size, length = keys.shape[1:]
    heads = head_bias.shape[0]
    steps = seqs // SEQ_STEP
    return pl.pallas_call(
        attend_kernel,
        out_shape=jax.ShapeDtypeStruct((seqs, width), BF16),
        in_specs=[pl.BlockSpec(memory_space=pl.ANY)] * 7,
        out_specs=whole(),
        scratch_shapes=[
            pltpu.SMEM((seqs,), jnp.int32),
            pltpu.SMEM((heads,), F32),
            VMEM(inputs.shape, BF16),
            VMEM(wq.shape, BF16),
            VMEM(keys.shape, BF16),
            VMEM(values.shape, BF16),
            VMEM(wo.shape, BF16),
            VMEM((seqs * heads, size), F32),
            VMEM((seqs * heads, size), F32),
            VMEM((CUM, CUM), BF16),
            pltpu.SemaphoreType.DMA((5,)),
            pltpu.SemaphoreType.DMA((steps,)),
            pltpu.SemaphoreType.DMA((steps,)),
        ],
        compiler_params=pltpu.CompilerParams(vmem_limit_bytes=36 * 2**20),
        cost_estimate=pl.CostEstimate(
            flops=8 * 10**9, bytes_accessed=22 * 10**6, transcendentals=2 * 10**6
        ),
        name="attend",
    )(*in_hbm(lengths, head_bias, inputs, wq, keys, values, wo))


def place_kernel(core_ref, routes_ref, place_ref, member_ref):
    choices, lanes = routes_ref.shape
    experts = member_ref.shape[0]
    rows = place_ref.shape[0]
    half = lanes // 2
    slots = rows // experts // 2
    expert = iota((experts, lanes), 0)
    named = expert == routes_ref[0:1, :]
    for k in range(1, choices):
        named = named | (expert == routes_ref[k : k + 1, :])
    member = jnp.where(named, 1.0, 0.0)
    member_ref[...] = member
    a, b = iota((lanes, lanes), 0), iota((lanes, lanes), 1)
    earlier = jnp.where((a < b) & ((a < half) == (b < half)), 1.0, 0.0).astype(BF16)
    slot = dot(member.astype(BF16), earlier)
    code = ((slot + 1.0) * member).astype(BF16)
    r, e = iota((rows, experts), 0), iota((rows, experts), 1)
    spread = jnp.where(r // (2 * slots) == e, 1.0, 0.0).astype(BF16)
    found = dot(spread, code)
    r, lane = iota((rows, lanes), 0), iota((rows, lanes), 1)
    wanted = (r % slots + 1 + core_ref[0] * slots).astype(F32)
    same_half = ((r // slots) % 2 == 0) == (lane < half)
    place_ref[...] = jnp.where((found == wanted) & same_half, 1.0, 0.0).astype(BF16)


def place(core, routes2, experts, slots):
    lanes = routes2.shape[1]
    return pl.pallas_call(
        place_kernel,
        out_shape=(
            jax.ShapeDtypeStruct((experts * 2 * slots, lanes), BF16),
            jax.ShapeDtypeStruct((experts, lanes), F32),
        ),
        in_specs=[pl.BlockSpec(memory_space=pltpu.SMEM), whole()],
        out_specs=(whole(), whole()),
        compiler_params=pltpu.CompilerParams(vmem_limit_bytes=8 * 2**20),
        cost_estimate=pl.CostEstimate(flops=10**8, bytes_accessed=10**5, transcendentals=0),
        name="place",
    )(core, routes2)


def halves(x):
    half = x.shape[1] // 2
    return jnp.concatenate([x[:, :half], x[:, half:]], axis=0)


def dispatch_kernel(
    x_ref, own_ref, other_ref, gain_ref, place_ref, hidden_hbm, out_hbm, hidden_scr, out_scr, sems
):
    v = (
        RESIDUAL_SCALE * x_ref[...].astype(F32)
        + own_ref[...].astype(F32)
        + other_ref[...].astype(F32)
    )
    centered = v - jnp.mean(v, axis=1, keepdims=True)
    var = jnp.mean(centered * centered, axis=1, keepdims=True)
    hidden = (centered * lax.rsqrt(var + NORM_EPS) * gain_ref[...]).astype(BF16)
    hidden_scr[...] = hidden
    copies = [pltpu.make_async_copy(hidden_scr, hidden_hbm, sems.at[PIECES])]
    copies[0].start()
    stacked = halves(hidden)
    rows = out_scr.shape[0] // PIECES
    for i in range(PIECES):
        part = pl.ds(i * rows, rows)
        out_scr[part, :] = dot(place_ref[part, :], stacked).astype(BF16)
        copies.append(pltpu.make_async_copy(out_scr.at[part], out_hbm.at[part], sems.at[i]))
        copies[-1].start()
    for copy in copies:
        copy.wait()


def dispatch(inputs, own, other, gain, placement):
    seqs, width = inputs.shape
    return pl.pallas_call(
        dispatch_kernel,
        out_shape=(
            pltpu.HBM((seqs, width), BF16),
            pltpu.HBM((placement.shape[0], width // 2), BF16),
        ),
        in_specs=[whole()] * 5,
        out_specs=(pl.BlockSpec(memory_space=pltpu.HBM),) * 2,
        scratch_shapes=[
            VMEM((seqs, width), BF16),
            VMEM((placement.shape[0], width // 2), BF16),
            pltpu.SemaphoreType.DMA((PIECES + 1,)),
        ],
        compiler_params=pltpu.CompilerParams(vmem_limit_bytes=12 * 2**20),
        cost_estimate=pl.CostEstimate(flops=2 * 10**8, bytes_accessed=2 * 10**6, transcendentals=64),
        name="dispatch",
    )(inputs, own, other, gain.reshape(1, width), placement)


def local_kernel(
    hidden_hbm, x_hbm, router_hbm, member_ref, place_ref, sg_hbm, su_hbm, sd_hbm, wk_hbm, wv_hbm,
    shared_ref, weight_ref, nk_ref, nv_ref, *scratch,
):
    *buffers, sems = scratch
    sources = [hidden_hbm, sg_hbm, su_hbm, sd_hbm, router_hbm, x_hbm, wk_hbm, wv_hbm]
    copies = [
        pltpu.make_async_copy(src, dst, sems.at[i])
        for i, (src, dst) in enumerate(zip(sources, buffers))
    ]
    for copy in copies:
        copy.start()
    hidden_ref, sg_ref, su_ref, sd_ref, router_ref, x_ref, wk_ref, wv_ref = buffers
    for copy in copies[:3]:
        copy.wait()
    hidden = hidden_ref[...]
    gate, up = dot(hidden, sg_ref[...]), dot(hidden, su_ref[...])
    inner = (gate / (1.0 + jnp.exp(-gate)) * up).astype(BF16)
    for copy in copies[3:]:
        copy.wait()
    shared_ref[...] = dot(inner, sd_ref[...])
    probs = 1.0 / (1.0 + jnp.exp(-dot_nt(router_ref[...], hidden)))
    probs = jnp.concatenate([probs, probs], axis=1) * member_ref[...]
    weights = ROUTE_SCALE * probs / jnp.sum(probs, axis=0, keepdims=True)
    experts = weights.shape[0]
    rows, lanes = place_ref.shape
    r, e = iota((rows, experts), 0), iota((rows, experts), 1)
    spread = jnp.where(r // (rows // experts) == e, 1.0, 0.0)
    placed = jnp.dot(spread, weights, precision=lax.Precision.HIGHEST, preferred_element_type=F32)
    placed = (placed * place_ref[...].astype(F32)).T
    high = placed.astype(BF16)
    weight_ref[:lanes, :] = high
    weight_ref[lanes:, :] = (placed - high.astype(F32)).astype(BF16)
    x = x_ref[...]
    nk_ref[...] = dot_nt(x, wk_ref[...]).astype(BF16)
    nv_ref[...] = dot_nt(x, wv_ref[...]).astype(BF16)


def local(hidden, inputs, router_t, member, placement, sg, su, sd, wk_t, wv_t):
    seqs, width = hidden.shape
    rows, lanes = placement.shape
    size = wk_t.shape[0]
    any_space = pl.BlockSpec(memory_space=pl.ANY)
    buffered = [hidden, sg, su, sd, router_t, inputs, wk_t, wv_t]
    return pl.pallas_call(
        local_kernel,
        out_shape=(
            jax.ShapeDtypeStruct((seqs, width), F32),
            jax.ShapeDtypeStruct((2 * lanes, rows), BF16),
            jax.ShapeDtypeStruct((seqs, size), BF16),
            jax.ShapeDtypeStruct((seqs, size), BF16),
        ),
        in_specs=[any_space] * 3 + [whole()] * 2 + [any_space] * 5,
        out_specs=(whole(),) * 4,
        scratch_shapes=[VMEM(b.shape, b.dtype) for b in buffered]
        + [pltpu.SemaphoreType.DMA((len(buffered),))],
        compiler_params=pltpu.CompilerParams(vmem_limit_bytes=24 * 2**20),
        cost_estimate=pl.CostEstimate(
            flops=4 * 10**9, bytes_accessed=5 * 10**6, transcendentals=10**5
        ),
        name="local",
    )(
        *in_hbm(hidden, inputs, router_t), member, placement, *in_hbm(sg, su, sd, wk_t, wv_t)
    )


def expert_kernel(
    order_ref, rows_ref, own_gate_ref, own_up_ref, down_hbm, gate2_hbm, up2_hbm, down2_hbm, out_ref,
    down_scr, gate2_scr, up2_scr, down2_scr, sems,
):
    sources = [gate2_hbm, up2_hbm, down_hbm, down2_hbm]
    buffers = [gate2_scr, up2_scr, down_scr, down2_scr]
    gate_copy, up_copy, *down_copies = [
        pltpu.make_async_copy(src, dst, sems.at[i])
        for i, (src, dst) in enumerate(zip(sources, buffers))
    ]
    gate_copy.start()
    up_copy.start()
    groups, lines, half = rows_ref.shape
    slots = lines // 2
    low = iota((groups // 2, lines, half), 1) < slots
    x = rows_ref[...].astype(F32).reshape(groups // 2, 2, lines, half)
    a, b = x[:, 0], x[:, 1]
    count = groups * slots
    first = jnp.where(low, a, pltpu.roll(b, slots, 1)).reshape(count, half).astype(BF16)
    second = jnp.where(low, pltpu.roll(a, slots, 1), b).reshape(count, half).astype(BF16)

    def product(ref):
        return dot(first, ref[:half, :]) + dot(second, ref[half:, :])

    def gated(gate, up):
        return (gate / (1.0 + jnp.exp(-gate)) * up).astype(BF16)

    gate, up = product(own_gate_ref), product(own_up_ref)
    for copy in down_copies:
        copy.start()
    own = gated(gate, up)
    gate_copy.wait()
    up_copy.wait()
    other = gated(product(gate2_scr), product(up2_scr))
    for copy in down_copies:
        copy.wait()

    def result(start):
        cols = slice(start, start + COLUMNS)
        parts = [
            dot(inner, ref[:, cols]).astype(BF16).astype(F32)
            for inner, ref in ((own, down_scr), (other, down2_scr))
        ]
        return (parts[0] + parts[1]).reshape(groups // 2, lines, COLUMNS)

    low = iota((groups // 2, lines, COLUMNS), 1) < slots
    for start in range(0, half, COLUMNS):
        a, b = result(start), result(half + start)
        even = jnp.where(low, a, pltpu.roll(b, slots, 1))
        odd = jnp.where(low, pltpu.roll(a, slots, 1), b)
        both = jnp.stack([even, odd], axis=1).reshape(groups, lines, COLUMNS)
        out_ref[:, :, start : start + COLUMNS] = both.astype(BF16)


def expert(order, rows, weights):
    gate, up, *streamed = weights
    any_space = pl.BlockSpec(memory_space=pl.ANY)
    return pl.pallas_call(
        expert_kernel,
        out_shape=jax.ShapeDtypeStruct(rows.shape, BF16),
        in_specs=[any_space] + [whole()] * 3 + [any_space] * 4,
        out_specs=whole(),
        scratch_shapes=[VMEM(w.shape, w.dtype) for w in streamed]
        + [pltpu.SemaphoreType.DMA((len(streamed),))],
        compiler_params=pltpu.CompilerParams(vmem_limit_bytes=32 * 2**20),
        cost_estimate=pl.CostEstimate(
            flops=2 * 10**9, bytes_accessed=8 * 10**6, transcendentals=3 * 10**5
        ),
        name="expert",
    )(*in_hbm(order), rows, gate, up, *in_hbm(*streamed))


def combine_kernel(weight_ref, rows_ref, shared_ref, hidden_ref, mine_ref, send_ref):
    lanes = weight_ref.shape[0] // 2
    both = dot(weight_ref[...], rows_ref[...])
    part = both[:lanes, :] + both[lanes:, :] + halves(shared_ref[...])
    send_ref[...] = part.astype(BF16)
    mine_ref[...] = part + RESIDUAL_SCALE * halves(hidden_ref[...]).astype(F32)


def combine(weight, rows, shared, hidden):
    shape = (weight.shape[0] // 2, rows.shape[1])
    return pl.pallas_call(
        combine_kernel,
        out_shape=(jax.ShapeDtypeStruct(shape, F32), jax.ShapeDtypeStruct(shape, BF16)),
        in_specs=[whole()] * 4,
        out_specs=(whole(), whole()),
        compiler_params=pltpu.CompilerParams(vmem_limit_bytes=16 * 2**20),
        cost_estimate=pl.CostEstimate(flops=3 * 10**8, bytes_accessed=3 * 10**6, transcendentals=0),
        name="combine",
    )(weight, rows, shared, hidden)


def finish_kernel(core_ref, mine_ref, other_ref, gain_ref, out_ref):
    seqs, half = out_ref.shape
    width = 2 * half
    v = mine_ref[...] + other_ref[...].astype(F32)
    sums = jnp.sum(v, axis=1, keepdims=True)
    squares = jnp.sum(v * v, axis=1, keepdims=True)
    mean = (sums[:seqs] + sums[seqs:]) / width
    var = (squares[:seqs] + squares[seqs:]) / width - mean * mean
    scale = lax.rsqrt(var + NORM_EPS)
    rows = pl.ds(pl.multiple_of(core_ref[0] * seqs, seqs), seqs)
    own = mine_ref[rows, :] + other_ref[rows, :].astype(F32)
    out_ref[...] = ((own - mean) * scale * gain_ref[...]).astype(BF16)


def finish(core, mine, other, gain):
    lanes, half = mine.shape
    return pl.pallas_call(
        finish_kernel,
        out_shape=jax.ShapeDtypeStruct((lanes // 2, half), BF16),
        in_specs=[pl.BlockSpec(memory_space=pltpu.SMEM)] + [whole()] * 3,
        out_specs=whole(),
        compiler_params=pltpu.CompilerParams(vmem_limit_bytes=12 * 2**20),
        cost_estimate=pl.CostEstimate(flops=10**7, bytes_accessed=2 * 10**6, transcendentals=64),
        name="finish",
    )(core, mine, other, gain.reshape(1, half))


def on_device(
    inputs,
    cache_keys,
    cache_values,
    lengths,
    query_weight,
    key_weight,
    value_weight,
    head_bias,
    out_weight,
    attend_gain,
    router_weight,
    routes,
    expert_gate,
    expert_up,
    expert_down,
    shared_gate,
    shared_up,
    shared_down,
    final_gain,
):
    seqs, width = inputs.shape
    experts = router_weight.shape[1]
    slots = 2 * seqs * routes.shape[1] // experts // 2
    core = lax.axis_index("tp").astype(jnp.int32).reshape(1)
    own_part = attend(
        inputs, cache_keys[:, 0], cache_values[:, 0], lengths, query_weight, head_bias, out_weight
    )
    other_part = swapped(own_part)
    routes_t = routes.T
    placement, member = place(core, jnp.concatenate([routes_t, routes_t], axis=1), experts, slots)
    hidden, outgoing = dispatch(inputs, own_part, other_part, attend_gain, placement)
    arrived = lax.all_to_all(
        outgoing.reshape(experts, 2 * slots, width // 2), "ep", 0, 0, tiled=True
    )
    own_weights = (expert_gate[0], expert_up[0], expert_down[0])
    other_weights = tuple(swapped(w) for w in own_weights)
    shared, weight, new_keys, new_values = local(
        hidden, inputs, router_weight.T, member, placement, shared_gate, shared_up, shared_down,
        key_weight.T, value_weight.T,
    )
    results = expert(new_keys, arrived, own_weights + other_weights)
    returned = lax.all_to_all(results, "ep", 0, 0, tiled=True)
    mine, send = combine(weight, returned.reshape(experts * 2 * slots, width // 2), shared, hidden)
    output = finish(core, mine, swapped(send), final_gain)
    return (output, new_keys, new_values)


def solution(mesh):
    placed = (
        P("ep", None),
        P("ep", "tp", None, None),
        P("ep", "tp", None, None),
        P("ep"),
        P(None, "tp"),
        P(None, "tp"),
        P(None, "tp"),
        P("tp"),
        P("tp", None),
        P(),
        P(),
        P("ep", None),
        P("ep", None, "tp"),
        P("ep", None, "tp"),
        P("ep", "tp", None),
        P(None, "tp"),
        P(None, "tp"),
        P("tp", None),
        P("tp"),
    )
    return jax.shard_map(
        on_device,
        mesh=mesh,
        in_specs=placed,
        out_specs=(P("ep", "tp"), P("ep", "tp"), P("ep", "tp")),
        check_vma=False,
    )
```
